32 devices in a mesh: ep: 8 (over z, x), tp: 4 (over y, core).
Axes of the slice: x: 2, y: 2, z: 4, core: 2. Of those that a mesh axis runs over, the one named last changes fastest.
Arguments:
- tokens: bfloat16 [6144, 2048], P(('ep', 'tp')), may hold values from -6 to 6
- routes: int32 [6144, 2], P(('ep', 'tp')), may hold values from 0 to 7, all different within a row; in each aligned block of 192 rows (0 to 191, 192 to 383, ...) at most 64 rows name the same one
- gates: float32 [6144, 2], P(('ep', 'tp')), may hold values from 0.3 to 2.2
- pre_gain: float32 [2048], replicated, may hold values from 0.1 to 1.9
- w_gate: bfloat16 [8, 2048, 512], P('ep'), may hold values from -0.125 to 0.125
- w_up: bfloat16 [8, 2048, 512], P('ep'), may hold values from -0.125 to 0.125
- w_down: bfloat16 [8, 512, 2048], P('ep'), may hold values from -0.25 to 0.25
- sh_gate: bfloat16 [2048, 512], P('tp'), may hold values from -0.125 to 0.125
- sh_up: bfloat16 [2048, 512], P('tp'), may hold values from -0.125 to 0.125
- sh_down: bfloat16 [512, 2048], P(None, 'tp'), may hold values from -0.25 to 0.25
- post_gain: float32 [2048], replicated, may hold values from 0.1 to 1.9
Outputs:
- mixed: bfloat16 [6144, 2048], P('ep', 'tp')
The draws below stay inside these ranges and needn't reach their ends.
Inputs may be any that keep to these rules, and one draw needn't show every extreme that they name: `routes`: each token names 2 different experts; among the rows of one device no expert is named more than 64 times, a bound that some block reaches.
All inputs are finite; a program needn't handle non-finite values.
Results may differ from the reference program's by a relative error of at most 0.0075.
Values may be sent and summed in bfloat16 or wider, within the bound.
A program may use at most 64 MiB of HBM per device.

```python
import math
import jax
import jax.numpy as jnp
import numpy as np
from jax import lax

D = 2048
FF = 512
SH = 512
TOPK = 2
TOK_DEV = 192
EXPERTS = 8
CAP = 64
TOKENS = 6144
N_EP = 8
N_TP = 4


def levels(key, shape, shards, smallest, largest):
    def one(axis_at, parts):
        draws = jax.random.uniform(jax.random.fold_in(jax.random.fold_in(key, 6), axis_at), (parts,), jnp.float32, smallest / len(shards), largest / len(shards))
        return jnp.repeat(jnp.exp(draws), shape[axis_at] // parts).reshape((-1,) + (1,) * (len(shape) - axis_at - 1))

    factor_of = one(*shards[0])
    for cut in shards[1:]:
        factor_of = factor_of * one(*cut)
    return factor_of


def assign_block(stream_key, own, number, rows, amount, top, limit, skew):
    ranking = jax.random.permutation(stream_key, amount)
    crowded, ordinary = portions_of(amount, rows * top, limit, skew, True), portions_of(amount, rows * top, limit, skew, False)
    places = jnp.arange(amount)

    def named(lengths, turn):
        used = int((lengths > 0).sum())
        fixed = max(1, used // 4)
        passed = fixed + (places - fixed + turn * (used - fixed)) % max(1, amount - fixed)
        return jnp.zeros((amount,), jnp.int32).at[ranking[jnp.where(places < fixed, places, passed)]].set(jnp.asarray(lengths, jnp.int32))

    lengths = jnp.where(number % 4 == 0, named(crowded, number // 4), named(ordinary, number - number // 4 - 1))
    mixed = jax.random.permutation(jax.random.fold_in(own, 3), amount)
    source_of, taker = mixed[0:amount // 2 * 2:2], mixed[1:amount // 2 * 2:2]
    margin = jnp.minimum(lengths[source_of] - 1, limit - lengths[taker]) // 2
    margin = jnp.where((source_of == ranking[0]) | (taker == ranking[0]) | (lengths[taker] == 0), 0, jnp.maximum(margin, 0))
    passed = jax.random.randint(jax.random.fold_in(own, 4), (amount // 2,), 0, 1 << 20) % (margin + 1)
    lengths = lengths.at[source_of].add(-passed).at[taker].add(passed)
    members = jnp.searchsorted(jnp.cumsum(lengths), jnp.arange(rows * top), side="right").astype(jnp.int32)
    grid = members.reshape(top, rows).T
    grid = grid[jax.random.permutation(jax.random.fold_in(own, 1), rows)]
    turn = jax.random.randint(jax.random.fold_in(own, 2), (rows, 1), 0, top)
    return jnp.take_along_axis(grid, (jnp.arange(top)[None, :] + turn) % top, axis=1)


def portions_of(count, total, limit, slope, full):
    portions = [(1 << 20) // math.isqrt(standing ** slope) + 1 for standing in range(1, count + 1)]
    largest = limit if full else min(limit, max(-(-total // count), total * portions[0] // sum(portions)))
    least = 1 if total - largest >= count - 1 else 0
    counts, spare = [largest] + [least] * (count - 1), total - largest - least * (count - 1)
    while spare > 0:
        free = [i for i in range(1, count) if counts[i] < largest] or [i for i in range(1, count) if counts[i] < limit]
        mass, remaining = sum([portions[i] for i in free]), spare
        for i in free:
            addition = min(limit - counts[i], max(1, remaining * portions[i] // mass), spare)
            counts[i] = counts[i] + addition
            spare = spare - addition
    return np.array(counts)


def normal_values(key, shape, scale, reach, split=(), kind=jnp.bfloat16):
    drawn = jax.random.normal(key, shape, jnp.float32) * scale
    if len(split) > 0:
        drawn = levels(key, shape, split, -0.22, 0.18) * drawn
    return jnp.clip(drawn, min=-reach, max=reach).astype(kind)


def setup_inputs(seed: int = 0) -> dict:
    key_of = jax.random.split(jax.random.key(seed), 12)
    tokens = normal_values(key_of[0], (TOKENS, D), 1.0, 6.0, ((0, 32),))
    routes_keys = jax.random.split(jax.random.fold_in(key_of[1], 1), TOKENS // TOK_DEV)
    routes_turns = jax.random.permutation(jax.random.fold_in(key_of[1], 3), TOKENS // TOK_DEV)
    routes = jax.vmap(lambda own, number: assign_block(jax.random.fold_in(key_of[1], 2), own, number, TOK_DEV, EXPERTS, TOPK, CAP, 2))(routes_keys, routes_turns).reshape((TOKENS, TOPK))
    gates = jnp.clip(0.3 + 1.90000004 * jax.random.uniform(key_of[2], (TOKENS, TOPK), jnp.float32) ** levels(key_of[2], (TOKENS, TOPK), ((0, 32),), -0.2, 0.2), 0.3, 2.2)
    pre_gain = jnp.clip(1.0 + 0.18 * jax.random.normal(key_of[3], (D,), jnp.float32), 0.1, 1.9)
    w_gate = normal_values(key_of[4], (EXPERTS, D, FF), D ** -0.5, 0.125, ((0, 8),))
    w_up = normal_values(key_of[5], (EXPERTS, D, FF), D ** -0.5, 0.125, ((0, 8),))
    w_down = normal_values(key_of[6], (EXPERTS, FF, D), FF ** -0.5, 0.25, ((0, 8),))
    sh_gate = normal_values(key_of[7], (D, SH), D ** -0.5, 0.125, ((0, 4),))
    sh_up = normal_values(key_of[8], (D, SH), D ** -0.5, 0.125, ((0, 4),))
    sh_down = normal_values(key_of[9], (SH, D), SH ** -0.5, 0.25, ((1, 4),))
    post_gain = jnp.clip(1.0 + 0.18 * jax.random.normal(key_of[10], (D,), jnp.float32), 0.1, 1.9)
    return dict(tokens=tokens, routes=routes, gates=gates, pre_gain=pre_gain, w_gate=w_gate, w_up=w_up, w_down=w_down, sh_gate=sh_gate, sh_up=sh_up, sh_down=sh_down, post_gain=post_gain)


def rms_scale(values):
    return lax.rsqrt(lax.optimization_barrier(jnp.mean(values * values, axis=-1, keepdims=True)) + 1e-06)

def reference(tokens, routes, gates, pre_gain, w_gate, w_up, w_down, sh_gate, sh_up, sh_down, post_gain):
    devices_all = N_EP * N_TP
    per_device = TOK_DEV * TOPK
    inputs = tokens.astype(jnp.float32)
    normed = (inputs * rms_scale(inputs) * pre_gain.astype(jnp.float32)).astype(jnp.bfloat16)
    expert_ids = routes.reshape(devices_all, per_device).astype(jnp.int32)
    matches = (expert_ids[:, :, None] == jnp.arange(EXPERTS, dtype=jnp.int32)[None, None, :]).astype(jnp.int32)
    earlier = jnp.cumsum(matches, axis=1) - matches
    slot_index = lax.optimization_barrier(jnp.sum(earlier * matches, axis=2)).astype(jnp.int32)
    sources = jnp.broadcast_to(jnp.arange(devices_all, dtype=jnp.int32)[:, None], (devices_all, per_device))
    token_index = sources * TOK_DEV + jnp.arange(per_device, dtype=jnp.int32)[None, :] // TOPK
    table = jnp.full((EXPERTS, devices_all, CAP), TOKENS, jnp.int32).at[expert_ids, sources, slot_index].set(token_index)
    weight_table = jnp.zeros((EXPERTS, devices_all, CAP), jnp.float32).at[expert_ids, sources, slot_index].set(gates.reshape(devices_all, per_device).astype(jnp.float32))
    padded = jnp.concatenate([normed, jnp.zeros((1, D), jnp.bfloat16)], axis=0)

    def one_expert(summed, pack):
        rows_index, row_weight, gate_mat, up_mat, down_mat = pack
        picked = padded[rows_index]
        gate_part = jnp.dot(picked, gate_mat, preferred_element_type=jnp.float32)
        up_part = jnp.dot(picked, up_mat, preferred_element_type=jnp.float32)
        hidden = (jax.nn.silu(gate_part) * up_part).astype(jnp.bfloat16)
        result = jnp.dot(hidden, down_mat, preferred_element_type=jnp.float32).astype(jnp.bfloat16)
        summed = summed.at[rows_index].add(row_weight[:, None] * result.astype(jnp.float32))
        return (summed, None)
    summed, _ = lax.scan(one_expert, jnp.zeros((TOKENS + 1, D), jnp.float32), (table.reshape(EXPERTS, -1), weight_table.reshape(EXPERTS, -1), w_gate, w_up, w_down))
    routed = summed[:TOKENS].astype(jnp.bfloat16)
    gate_shared = jnp.dot(normed, sh_gate, preferred_element_type=jnp.float32)
    up_shared = jnp.dot(normed, sh_up, preferred_element_type=jnp.float32)
    shared_hidden = (jax.nn.silu(gate_shared) * up_shared).astype(jnp.bfloat16)
    shared = jnp.dot(shared_hidden, sh_down, preferred_element_type=jnp.float32).astype(jnp.bfloat16)
    combined = routed.astype(jnp.float32) + shared.astype(jnp.float32)
    return (combined * rms_scale(combined) * post_gain.astype(jnp.float32)).astype(jnp.bfloat16)
```

```python
import functools

import jax
import jax.numpy as jnp
from jax import lax
from jax.experimental import pallas as pl
from jax.experimental.pallas import tpu as pltpu
from jax.sharding import PartitionSpec as P

TOPK = 2
F32 = jnp.float32
BF16 = jnp.bfloat16
MESH = pl.DeviceIdType.MESH


def silu(v):
    return v / (1.0 + jnp.exp(-v))


def dot(a, b):
    return jnp.dot(a, b, preferred_element_type=F32)


def kernel(
    n, tp, cap,
    tokens, routes, gates, pre_gain, post_gain, w_gate, w_up, w_down, sh_gate, sh_up, sh_down,
    out,
    normed, key, pick, send, recv, res, ret, wg, wu, wd, sg, su, sd, acc, shared, obuf,
    load_sem, d_send, d_recv, r_send, r_recv, s_send, s_recv, o_send, o_recv,
):
    rows, width = tokens.shape
    block = 32 if rows % 32 == 0 else rows
    cols = width // tp
    me = lax.axis_index("ep")
    mt = lax.axis_index("tp")
    half = n // 2
    mine = lax.rem(me, half)
    near = me - mine
    far = lax.rem(near + half, n)

    barrier = pltpu.get_barrier_semaphore()

    def greet_ep(k, c):
        pl.semaphore_signal(
            barrier, inc=1, device_id={"ep": lax.rem(me + k, n)}, device_id_type=MESH
        )
        return c

    def greet_tp(k, c):
        pl.semaphore_signal(
            barrier, inc=1, device_id={"tp": lax.rem(mt + k, tp)}, device_id_type=MESH
        )
        return c

    lax.fori_loop(1, n, greet_ep, 0)
    lax.fori_loop(1, tp, greet_tp, 0)

    loads = [
        pltpu.make_async_copy(src, dst, load_sem.at[i])
        for i, (src, dst) in enumerate(
            (
                (w_gate.at[0], wg),
                (w_up.at[0], wu),
                (w_down.at[0], wd),
                (sh_gate, sg.at[mt]),
                (sh_up, su.at[mt]),
                (sh_down, sd.at[mt]),
            )
        )
    ]
    for load in loads:
        load.start()

    def norm_rows(i, c):
        at = pl.ds(pl.multiple_of(i * block, block), block)
        v = tokens[at, :].astype(F32)
        scale = lax.rsqrt(jnp.mean(v * v, axis=1, keepdims=True) + 1e-06)
        normed[at, :] = (v * scale * pre_gain[...]).astype(BF16)
        return c

    lax.fori_loop(0, rows // block, norm_rows, 0)

    lanes = key.shape[0]
    expert = lax.broadcasted_iota(jnp.int32, (rows, lanes), 1)
    named = (routes[:, 0:1] == expert) | (routes[:, 1:2] == expert)
    named = jnp.where(named, 1.0, 0.0).astype(BF16)
    row = lax.broadcasted_iota(jnp.int32, (rows, rows), 0)
    column = lax.broadcasted_iota(jnp.int32, (rows, rows), 1)
    before = jnp.where(row < column, 1.0, 0.0).astype(BF16)
    same = jnp.where(row == column, 1.0, 0.0).astype(BF16)
    over_rows = (((0,), (0,)), ((), ()))
    rank = lax.dot_general(named, before, over_rows, preferred_element_type=F32)
    named_t = lax.dot_general(named, same, over_rows, preferred_element_type=F32)
    key[...] = jnp.where(named_t > 0.5, rank, -1.0)
    slot = lax.broadcasted_iota(jnp.int32, (cap, rows), 0).astype(F32)

    def fill(d):
        chosen = jnp.where(slot == key[pl.ds(d, 1), :], 1.0, 0.0).astype(BF16)
        pick[d] = chosen
        send[d] = dot(chosen, normed[...]).astype(BF16)

    def dispatch(d, s):
        return pltpu.make_async_remote_copy(
            src_ref=send.at[d], dst_ref=recv.at[s],
            send_sem=d_send.at[d], recv_sem=d_recv.at[s],
            device_id={"ep": d}, device_id_type=MESH,
        )

    def giveback(s, e):
        return pltpu.make_async_remote_copy(
            src_ref=res.at[s], dst_ref=ret.at[e],
            send_sem=r_send.at[s], recv_sem=r_recv.at[e],
            device_id={"ep": s}, device_id_type=MESH,
        )

    def share(which, d, s):
        src, dst = ((sh_gate, sg), (sh_up, su), (sh_down, sd))[which]
        return pltpu.make_async_remote_copy(
            src_ref=src, dst_ref=dst.at[s],
            send_sem=s_send.at[which, d], recv_sem=s_recv.at[which, s],
            device_id={"tp": d}, device_id_type=MESH,
        )

    def emit(d, s):
        return pltpu.make_async_remote_copy(
            src_ref=obuf.at[d], dst_ref=out.at[pl.ds(pl.multiple_of(s * rows, rows), rows), :],
            send_sem=o_send.at[d], recv_sem=o_recv.at[s],
            device_id={"tp": d}, device_id_type=MESH,
        )

    fill(far + mine)
    pl.semaphore_wait(barrier, n - 1 + tp - 1)
    dispatch(far + mine, me).start()

    def send_far(j, c):
        d = far + lax.rem(mine + j, half)
        fill(d)
        dispatch(d, me).start()
        return c

    def send_near(j, c):
        d = near + lax.rem(mine + j, half)
        fill(d)
        dispatch(d, me).start()
        return c

    lax.fori_loop(1, half, send_far, 0)
    for which in range(3):
        def send_shared(k, c):
            share(which, lax.rem(mt + k, tp), mt).start()
            return c

        lax.fori_loop(1, tp, send_shared, 0)
    lax.fori_loop(1, half, send_near, 0)
    fill(me)

    for load in loads[:3]:
        load.wait()

    def run(x):
        hidden = (silu(dot(x, wg[...])) * dot(x, wu[...])).astype(BF16)
        return dot(hidden, wd[...]).astype(BF16)

    ret[me] = run(send[me])

    def serve(s):
        dispatch(me, s).wait_recv()
        res[s] = run(recv[s])
        giveback(s, me).start()

    def serve_far(j, c):
        serve(far + lax.rem(mine + half - j, half))
        return c

    def serve_near(j, c):
        serve(near + lax.rem(mine + half - j, half))
        return c

    lax.fori_loop(0, half, serve_far, 0)
    lax.fori_loop(1, half, serve_near, 0)

    def weight_of(e):
        first = jnp.where(routes[:, 0:1] == e, gates[:, 0:1], 0.0)
        return first + jnp.where(routes[:, 1:2] == e, gates[:, 1:2], 0.0)

    def placed(e):
        rowsof = lax.dot_general(pick[e], ret[e], over_rows, preferred_element_type=F32)
        return weight_of(e) * rowsof

    acc[...] = placed(me)

    for load in loads[3:]:
        load.wait()

    def arrive(which):
        def one(k, c):
            share(which, mt, lax.rem(mt + tp - k, tp)).wait_recv()
            return c

        lax.fori_loop(1, tp, one, 0)

    arrive(0)
    arrive(1)
    full = (width, sg.shape[2])
    gate_shared = dot(normed[...], sg[...].reshape(full))
    up_shared = dot(normed[...], su[...].reshape(full))
    shared_hidden = (silu(gate_shared) * up_shared).astype(BF16)
    arrive(2)

    def project(t, c):
        at = pl.ds(pl.multiple_of(t * cols, cols), cols)
        shared[:, at] = dot(shared_hidden, sd[t]).astype(BF16)
        return c

    lax.fori_loop(0, tp, project, 0)

    def gather_far(j, c):
        e = far + lax.rem(mine + j, half)
        giveback(me, e).wait_recv()
        acc[...] += placed(e)
        return c

    def gather_near(j, c):
        e = near + lax.rem(mine + j, half)
        giveback(me, e).wait_recv()
        acc[...] += placed(e)
        return c

    lax.fori_loop(1, half, gather_near, 0)
    lax.fori_loop(0, half, gather_far, 0)

    def finish(i, c):
        at = pl.ds(pl.multiple_of(i * block, block), block)
        combined = acc[at, :].astype(BF16).astype(F32) + shared[at, :].astype(F32)
        scale = lax.rsqrt(jnp.mean(combined * combined, axis=1, keepdims=True) + 1e-06)
        mixed = (combined * scale * post_gain[...]).astype(BF16)
        for t in range(tp):
            obuf[t, at, :] = mixed[:, t * cols : (t + 1) * cols]
        return c

    lax.fori_loop(0, rows // block, finish, 0)

    def send_out(k, c):
        emit(lax.rem(mt + k, tp), mt).start()
        return c

    lax.fori_loop(1, tp, send_out, 0)
    out[pl.ds(pl.multiple_of(mt * rows, rows), rows), :] = obuf[mt]

    def drain_far(j, c):
        d = far + lax.rem(mine + j, half)
        dispatch(d, me).wait_send()
        giveback(d, me).wait_send()
        return c

    def drain_near(j, c):
        d = near + lax.rem(mine + j, half)
        dispatch(d, me).wait_send()
        giveback(d, me).wait_send()
        return c

    lax.fori_loop(0, half, drain_far, 0)
    lax.fori_loop(1, half, drain_near, 0)

    def drain_tp(k, c):
        d = lax.rem(mt + k, tp)
        for which in range(3):
            share(which, d, mt).wait_send()
        emit(d, mt).wait_send()
        emit(mt, d).wait_recv()
        return c

    lax.fori_loop(1, tp, drain_tp, 0)


def per_device(
    tokens, routes, gates, pre_gain, w_gate, w_up, w_down, sh_gate, sh_up, sh_down, post_gain
):
    rows, width = tokens.shape
    n = lax.axis_size("ep")
    tp = lax.axis_size("tp")
    cap = -(-max(2, 4 * rows * TOPK // (3 * n)) // 16) * 16
    lanes = -(-n // 128) * 128
    hidden = w_gate.shape[2]
    sh = sh_gate.shape[1]
    cols = width // tp
    vmem = pl.BlockSpec(memory_space=pltpu.VMEM)
    hbm = pl.BlockSpec(memory_space=pl.ANY)
    dma = pltpu.SemaphoreType.DMA
    return pl.pallas_call(
        functools.partial(kernel, n, tp, cap),
        out_shape=jax.ShapeDtypeStruct((tp * rows, cols), BF16),
        in_specs=[vmem] * 5 + [hbm] * 6,
        out_specs=vmem,
        scratch_shapes=[
            pltpu.VMEM((rows, width), BF16),
            pltpu.VMEM((lanes, rows), F32),
            pltpu.VMEM((n, cap, rows), BF16),
            pltpu.VMEM((n, cap, width), BF16),
            pltpu.VMEM((n, cap, width), BF16),
            pltpu.VMEM((n, cap, width), BF16),
            pltpu.VMEM((n, cap, width), BF16),
            pltpu.VMEM((width, hidden), BF16),
            pltpu.VMEM((width, hidden), BF16),
            pltpu.VMEM((hidden, width), BF16),
            pltpu.VMEM((tp, width // tp, sh), BF16),
            pltpu.VMEM((tp, width // tp, sh), BF16),
            pltpu.VMEM((tp, sh, cols), BF16),
            pltpu.VMEM((rows, width), F32),
            pltpu.VMEM((rows, width), BF16),
            pltpu.VMEM((tp, rows, cols), BF16),
            dma((6,)),
            dma((n,)), dma((n,)), dma((n,)), dma((n,)),
            dma((3, tp)), dma((3, tp)),
            dma((tp,)), dma((tp,)),
        ],
        compiler_params=pltpu.CompilerParams(
            collective_id=0, has_side_effects=True, vmem_limit_bytes=56 * 1024 * 1024
        ),
    )(
        tokens, routes, gates, pre_gain.reshape(1, width), post_gain.reshape(1, width),
        w_gate, w_up, w_down, sh_gate, sh_up, sh_down,
    )


def solution(mesh):
    return jax.shard_map(
        per_device,
        mesh=mesh,
        in_specs=(
            P(("ep", "tp"), None),
            P(("ep", "tp"), None),
            P(("ep", "tp"), None),
            P(),
            P("ep", None, None),
            P("ep", None, None),
            P("ep", None, None),
            P("tp", None),
            P("tp", None),
            P(None, "tp"),
            P(),
        ),
        out_specs=P("ep", "tp"),
        check_vma=False,
    )
```

```python
import functools

import jax
import jax.numpy as jnp
from jax import lax
from jax.experimental import pallas as pl
from jax.experimental.pallas import tpu as pltpu
from jax.sharding import PartitionSpec as P

TOPK = 2
F32 = jnp.float32
BF16 = jnp.bfloat16
MESH = pl.DeviceIdType.MESH


def silu(v):
    return v / (1.0 + jnp.exp(-v))


def dot(a, b):
    return jnp.dot(a, b, preferred_element_type=F32)


def kernel(
    n, tp, cap,
    tokens, routes, gates, pre_gain, post_gain, w_gate, w_up, w_down, sh_gate, sh_up, sh_down,
    out,
    normed, key, pick, send, recv, res, ret, wg, wu, wd, sg, su, sd, acc, shared,
    routes_all, gates_all, hidden_all, sums,
    load_sem, d_send, d_recv, r_send, r_recv, s_send, s_recv,
):
    rows, width = tokens.shape
    block = 32 if rows % 32 == 0 else rows
    cols = width // tp
    me = lax.axis_index("ep")
    mt = lax.axis_index("tp")
    half = n // 2
    mine = lax.rem(me, half)
    near = me - mine
    far = lax.rem(near + half, n)

    barrier = pltpu.get_barrier_semaphore()

    def greet(k, c):
        flat = lax.rem(me * tp + mt + k, n * tp)
        pl.semaphore_signal(
            barrier, inc=1, device_id={"ep": flat // tp, "tp": lax.rem(flat, tp)},
            device_id_type=MESH,
        )
        return c

    lax.fori_loop(1, n * tp, greet, 0)

    loads = [
        pltpu.make_async_copy(src, dst, load_sem.at[i])
        for i, (src, dst) in enumerate(
            (
                (w_gate.at[0], wg),
                (w_up.at[0], wu),
                (w_down.at[0], wd),
                (sh_gate, sg.at[mt]),
                (sh_up, su.at[mt]),
                (sh_down, sd),
            )
        )
    ]
    for load in loads:
        load.start()

    def norm_rows(i, c):
        at = pl.ds(pl.multiple_of(i * block, block), block)
        v = tokens[at, :].astype(F32)
        scale = lax.rsqrt(jnp.mean(v * v, axis=1, keepdims=True) + 1e-06)
        normed[at, :] = (v * scale * pre_gain[...]).astype(BF16)
        return c

    lax.fori_loop(0, rows // block, norm_rows, 0)

    lanes = key.shape[1]
    row = lax.broadcasted_iota(jnp.int32, (rows, rows), 0)
    column = lax.broadcasted_iota(jnp.int32, (rows, rows), 1)
    before = jnp.where(row < column, 1.0, 0.0).astype(BF16)
    same = jnp.where(row == column, 1.0, 0.0).astype(BF16)
    over_rows = (((0,), (0,)), ((), ()))
    slot = lax.broadcasted_iota(jnp.int32, (cap, rows), 0).astype(F32)

    def index(t):
        expert = lax.broadcasted_iota(jnp.int32, (rows, lanes), 1)
        ids = routes_all[t]
        named = (ids[:, 0:1] == expert) | (ids[:, 1:2] == expert)
        named = jnp.where(named, 1.0, 0.0).astype(BF16)
        rank = lax.dot_general(named, before, over_rows, preferred_element_type=F32)
        named_t = lax.dot_general(named, same, over_rows, preferred_element_type=F32)
        key[t] = jnp.where(named_t > 0.5, rank, -1.0)

    def choose(t, e):
        chosen = jnp.where(slot == key[t, pl.ds(e, 1), :], 1.0, 0.0).astype(BF16)
        pick[t, e] = chosen
        return chosen

    routes_all[mt] = routes[...]
    gates_all[mt] = gates[...]
    index(mt)

    def fill(d):
        send[d] = dot(choose(mt, d), normed[...]).astype(BF16)

    def dispatch(d, s):
        return pltpu.make_async_remote_copy(
            src_ref=send.at[d], dst_ref=recv.at[s],
            send_sem=d_send.at[d], recv_sem=d_recv.at[s],
            device_id={"ep": d}, device_id_type=MESH,
        )

    def giveback(s, t, e, u):
        return pltpu.make_async_remote_copy(
            src_ref=res.at[s, t], dst_ref=ret.at[e, u],
            send_sem=r_send.at[s, t], recv_sem=r_recv.at[e, u],
            device_id={"ep": s, "tp": t}, device_id_type=MESH,
        )

    def share(which, d, s):
        src, dst = (
            (sh_gate, sg.at[s]),
            (sh_up, su.at[s]),
            (hidden_all.at[mt], hidden_all.at[s]),
            (routes, routes_all.at[s]),
            (gates, gates_all.at[s]),
            (sums.at[mt], sums.at[s]),
        )[which]
        return pltpu.make_async_remote_copy(
            src_ref=src, dst_ref=dst,
            send_sem=s_send.at[which, d], recv_sem=s_recv.at[which, s],
            device_id={"tp": d}, device_id_type=MESH,
        )

    def spread(which):
        def one(k, c):
            share(which, lax.rem(mt + k, tp), mt).start()
            return c

        lax.fori_loop(1, tp, one, 0)

    def arrive(which):
        def one(k, c):
            share(which, mt, lax.rem(mt + tp - k, tp)).wait_recv()
            return c

        lax.fori_loop(1, tp, one, 0)

    fill(far + mine)
    pl.semaphore_wait(barrier, n * tp - 1)
    dispatch(far + mine, me).start()

    def send_far(j, c):
        d = far + lax.rem(mine + j, half)
        fill(d)
        dispatch(d, me).start()
        return c

    def send_near(j, c):
        d = near + lax.rem(mine + j, half)
        fill(d)
        dispatch(d, me).start()
        return c

    lax.fori_loop(1, half, send_far, 0)
    spread(3)
    spread(4)
    spread(0)
    spread(1)
    lax.fori_loop(1, half, send_near, 0)
    fill(me)

    for load in loads[:3]:
        load.wait()

    def run(x):
        hidden = (silu(dot(x, wg[...])) * dot(x, wu[...])).astype(BF16)
        return dot(hidden, wd[...]).astype(BF16)

    def split(s, result):
        for t in range(tp):
            res[s, t] = result[:, t * cols : (t + 1) * cols]

    def send_back(s, first):
        def one(k, c):
            giveback(s, lax.rem(mt + k, tp), me, mt).start()
            return c

        lax.fori_loop(first, tp, one, 0)

    split(me, run(send[me]))
    send_back(me, 1)
    ret[me, mt] = res[me, mt]

    arrive(3)
    arrive(4)

    def index_other(k, c):
        t = lax.rem(mt + k, tp)
        index(t)

        def each(e, c):
            choose(t, e)
            return c

        lax.fori_loop(0, n, each, 0)
        return c

    lax.fori_loop(1, tp, index_other, 0)

    def serve(s):
        dispatch(me, s).wait_recv()
        split(s, run(recv[s]))
        send_back(s, 0)

    def serve_far(j, c):
        serve(far + lax.rem(mine + half - j, half))
        return c

    def serve_near(j, c):
        serve(near + lax.rem(mine + half - j, half))
        return c

    lax.fori_loop(0, half, serve_far, 0)
    lax.fori_loop(1, half, serve_near, 0)

    for load in loads[3:]:
        load.wait()
    arrive(0)
    arrive(1)
    full = (width, sg.shape[2])
    gate_shared = dot(normed[...], sg[...].reshape(full))
    up_shared = dot(normed[...], su[...].reshape(full))
    hidden_all[mt] = (silu(gate_shared) * up_shared).astype(BF16)
    spread(2)

    def placed(e, t):
        ids, gains = routes_all[t], gates_all[t]
        weight = jnp.where(ids[:, 0:1] == e, gains[:, 0:1], 0.0)
        weight = weight + jnp.where(ids[:, 1:2] == e, gains[:, 1:2], 0.0)
        rowsof = lax.dot_general(pick[t, e], ret[e, t], over_rows, preferred_element_type=F32)
        return weight * rowsof

    acc[mt] = placed(me, mt)

    def gather_own(k, c):
        t = lax.rem(mt + tp - k, tp)
        giveback(me, mt, me, t).wait_recv()
        acc[t] = placed(me, t)
        return c

    lax.fori_loop(1, tp, gather_own, 0)

    def gather(e):
        def one(k, c):
            t = lax.rem(mt + tp - k, tp)
            giveback(me, mt, e, t).wait_recv()
            acc[t] += placed(e, t)
            return c

        lax.fori_loop(0, tp, one, 0)

    def gather_far(j, c):
        gather(far + lax.rem(mine + j, half))
        return c

    def gather_near(j, c):
        gather(near + lax.rem(mine + j, half))
        return c

    lax.fori_loop(1, half, gather_near, 0)
    arrive(2)

    def project(t, c):
        shared[t] = dot(hidden_all[t], sd[...]).astype(BF16)
        return c

    lax.fori_loop(0, tp, project, 0)
    lax.fori_loop(0, half, gather_far, 0)

    def total(t, c):
        combined = acc[t].astype(BF16).astype(F32) + shared[t].astype(F32)
        acc[t] = combined
        squares = jnp.sum(combined * combined, axis=1, keepdims=True)
        sums[mt, t] = jnp.broadcast_to(squares, (rows, 128)).T[0:8, :]
        return c

    lax.fori_loop(0, tp, total, 0)
    spread(5)
    arrive(5)

    def finish(t, c):
        squares = sums[0, t]
        for u in range(1, tp):
            squares = squares + sums[u, t]
        squares = jnp.broadcast_to(squares[0:1, :], (128, rows)).T[:, 0:1]
        scale = lax.rsqrt(squares * (1.0 / width) + 1e-06)
        at = pl.ds(pl.multiple_of(t * rows, rows), rows)
        out[at, :] = (acc[t] * scale * post_gain[mt]).astype(BF16)
        return c

    lax.fori_loop(0, tp, finish, 0)

    def drain(d, first):
        def one(k, c):
            giveback(d, lax.rem(mt + k, tp), me, mt).wait_send()
            return c

        lax.fori_loop(first, tp, one, 0)

    def drain_far(j, c):
        d = far + lax.rem(mine + j, half)
        dispatch(d, me).wait_send()
        drain(d, 0)
        return c

    def drain_near(j, c):
        d = near + lax.rem(mine + j, half)
        dispatch(d, me).wait_send()
        drain(d, 0)
        return c

    drain(me, 1)
    lax.fori_loop(0, half, drain_far, 0)
    lax.fori_loop(1, half, drain_near, 0)

    def drain_tp(k, c):
        d = lax.rem(mt + k, tp)
        for which in range(6):
            share(which, d, mt).wait_send()
        return c

    lax.fori_loop(1, tp, drain_tp, 0)


def per_device(
    tokens, routes, gates, pre_gain, w_gate, w_up, w_down, sh_gate, sh_up, sh_down, post_gain
):
    rows, width = tokens.shape
    n = lax.axis_size("ep")
    tp = lax.axis_size("tp")
    cap = -(-max(2, 4 * rows * TOPK // (3 * n)) // 16) * 16
    lanes = -(-n // 128) * 128
    hidden = w_gate.shape[2]
    sh = sh_gate.shape[1]
    cols = width // tp
    vmem = pl.BlockSpec(memory_space=pltpu.VMEM)
    hbm = pl.BlockSpec(memory_space=pl.ANY)
    dma = pltpu.SemaphoreType.DMA
    return pl.pallas_call(
        functools.partial(kernel, n, tp, cap),
        out_shape=jax.ShapeDtypeStruct((tp * rows, cols), BF16),
        in_specs=[vmem] * 5 + [hbm] * 6,
        out_specs=vmem,
        scratch_shapes=[
            pltpu.VMEM((rows, width), BF16),
            pltpu.VMEM((tp, lanes, rows), F32),
            pltpu.VMEM((tp, n, cap, rows), BF16),
            pltpu.VMEM((n, cap, width), BF16),
            pltpu.VMEM((n, cap, width), BF16),
            pltpu.VMEM((n, tp, cap, cols), BF16),
            pltpu.VMEM((n, tp, cap, cols), BF16),
            pltpu.VMEM((width, hidden), BF16),
            pltpu.VMEM((width, hidden), BF16),
            pltpu.VMEM((hidden, width), BF16),
            pltpu.VMEM((tp, width // tp, sh), BF16),
            pltpu.VMEM((tp, width // tp, sh), BF16),
            pltpu.VMEM((sh, cols), BF16),
            pltpu.VMEM((tp, rows, cols), F32),
            pltpu.VMEM((tp, rows, cols), BF16),
            pltpu.VMEM((tp, rows, TOPK), jnp.int32),
            pltpu.VMEM((tp, rows, TOPK), F32),
            pltpu.VMEM((tp, rows, sh), BF16),
            pltpu.VMEM((tp, tp, 8, rows), F32),
            dma((6,)),
            dma((n,)), dma((n,)), dma((n, tp)), dma((n, tp)),
            dma((6, tp)), dma((6, tp)),
        ],
        compiler_params=pltpu.CompilerParams(
            collective_id=0, has_side_effects=True, vmem_limit_bytes=56 * 1024 * 1024
        ),
    )(
        tokens, routes, gates, pre_gain.reshape(1, width), post_gain.reshape(tp, 1, cols),
        w_gate, w_up, w_down, sh_gate, sh_up, sh_down,
    )


def solution(mesh):
    return jax.shard_map(
        per_device,
        mesh=mesh,
        in_specs=(
            P(("ep", "tp"), None),
            P(("ep", "tp"), None),
            P(("ep", "tp"), None),
            P(),
            P("ep", None, None),
            P("ep", None, None),
            P("ep", None, None),
            P("tp", None),
            P("tp", None),
            P(None, "tp"),
            P(),
        ),
        out_specs=P("ep", "tp"),
        check_vma=False,
    )
```

```python
import functools

import jax
import jax.numpy as jnp
from jax import lax
from jax.experimental import pallas as pl
from jax.experimental.pallas import tpu as pltpu
from jax.sharding import PartitionSpec as P

TOPK = 2
F32 = jnp.float32
BF16 = jnp.bfloat16
MESH = pl.DeviceIdType.MESH


def silu(v):
    return v / (1.0 + jnp.exp(-v))


def dot(a, b):
    return jnp.dot(a, b, preferred_element_type=F32)


def kernel(
    n, tp, cap,
    tokens, routes, gates, pre_gain, post_gain, w_gate, w_up, w_down, sh_gate, sh_up, sh_down,
    out,
    normed, key, pick, send, recv, res, ret, wg, wu, wd, sg, su, sd, acc, shared,
    routes_all, gates_all, hidden_all, sums,
    load_sem, d_send, d_recv, r_send, r_recv, s_send, s_recv,
):
    rows, width = tokens.shape
    block = 32 if rows % 32 == 0 else rows
    cols = width // tp
    me = lax.axis_index("ep")
    mt = lax.axis_index("tp")
    half = n // 2
    mine = lax.rem(me, half)
    near = me - mine
    far = lax.rem(near + half, n)

    barrier = pltpu.get_barrier_semaphore()

    def greet(k, c):
        flat = lax.rem(me * tp + mt + k, n * tp)
        pl.semaphore_signal(
            barrier, inc=1, device_id={"ep": flat // tp, "tp": lax.rem(flat, tp)},
            device_id_type=MESH,
        )
        return c

    lax.fori_loop(1, n * tp, greet, 0)

    loads = [
        pltpu.make_async_copy(src, dst, load_sem.at[i])
        for i, (src, dst) in enumerate(
            (
                (w_gate.at[0], wg),
                (w_up.at[0], wu),
                (w_down.at[0], wd),
                (sh_gate, sg.at[mt]),
                (sh_up, su.at[mt]),
                (sh_down, sd),
            )
        )
    ]
    for load in loads:
        load.start()

    def norm_rows(i, c):
        at = pl.ds(pl.multiple_of(i * block, block), block)
        v = tokens[at, :].astype(F32)
        scale = lax.rsqrt(jnp.mean(v * v, axis=1, keepdims=True) + 1e-06)
        normed[at, :] = (v * scale * pre_gain[...]).astype(BF16)
        return c

    lax.fori_loop(0, rows // block, norm_rows, 0)

    lanes = key.shape[1]
    row = lax.broadcasted_iota(jnp.int32, (rows, rows), 0)
    column = lax.broadcasted_iota(jnp.int32, (rows, rows), 1)
    before = jnp.where(row < column, 1.0, 0.0).astype(BF16)
    same = jnp.where(row == column, 1.0, 0.0).astype(BF16)
    over_rows = (((0,), (0,)), ((), ()))
    slot = lax.broadcasted_iota(jnp.int32, (cap, rows), 0).astype(F32)

    def index(t):
        expert = lax.broadcasted_iota(jnp.int32, (rows, lanes), 1)
        ids = routes_all[t]
        named = (ids[:, 0:1] == expert) | (ids[:, 1:2] == expert)
        named = jnp.where(named, 1.0, 0.0).astype(BF16)
        rank = lax.dot_general(named, before, over_rows, preferred_element_type=F32)
        named_t = lax.dot_general(named, same, over_rows, preferred_element_type=F32)
        key[t] = jnp.where(named_t > 0.5, rank, -1.0)

    def choose(t, e):
        chosen = jnp.where(slot == key[t, pl.ds(e, 1), :], 1.0, 0.0).astype(BF16)
        pick[t, e] = chosen
        return chosen

    routes_all[mt] = routes[...]
    gates_all[mt] = gates[...]
    index(mt)

    def fill(d):
        send[d] = dot(choose(mt, d), normed[...]).astype(BF16)

    def dispatch(d, s):
        return pltpu.make_async_remote_copy(
            src_ref=send.at[d], dst_ref=recv.at[s],
            send_sem=d_send.at[d], recv_sem=d_recv.at[s],
            device_id={"ep": d}, device_id_type=MESH,
        )

    def giveback(s, t, e, u):
        return pltpu.make_async_remote_copy(
            src_ref=res.at[s, t], dst_ref=ret.at[e, u],
            send_sem=r_send.at[s, t], recv_sem=r_recv.at[e, u],
            device_id={"ep": s, "tp": t}, device_id_type=MESH,
        )

    def share(which, d, s):
        src, dst = (
            (sh_gate, sg.at[s]),
            (sh_up, su.at[s]),
            (hidden_all.at[mt], hidden_all.at[s]),
            (routes, routes_all.at[s]),
            (gates, gates_all.at[s]),
            (sums.at[mt], sums.at[s]),
        )[which]
        return pltpu.make_async_remote_copy(
            src_ref=src, dst_ref=dst,
            send_sem=s_send.at[which, d], recv_sem=s_recv.at[which, s],
            device_id={"tp": d}, device_id_type=MESH,
        )

    def spread(which):
        def one(k, c):
            share(which, lax.rem(mt + k, tp), mt).start()
            return c

        lax.fori_loop(1, tp, one, 0)

    def arrive(which):
        def one(k, c):
            share(which, mt, lax.rem(mt + tp - k, tp)).wait_recv()
            return c

        lax.fori_loop(1, tp, one, 0)

    fill(far + mine)
    pl.semaphore_wait(barrier, n * tp - 1)
    dispatch(far + mine, me).start()

    def send_far(j, c):
        d = far + lax.rem(mine + j, half)
        fill(d)
        dispatch(d, me).start()
        return c

    def send_near(j, c):
        d = near + lax.rem(mine + j, half)
        fill(d)
        dispatch(d, me).start()
        return c

    def send_both(j, c):
        send_near(j, c)
        return send_far(j, c)

    lax.fori_loop(1, half, send_both, 0)
    spread(3)
    spread(4)
    spread(0)
    spread(1)
    fill(me)

    for load in loads[:3]:
        load.wait()

    def run(x):
        hidden = (silu(dot(x, wg[...])) * dot(x, wu[...])).astype(BF16)
        return dot(hidden, wd[...]).astype(BF16)

    def split(s, result):
        for t in range(tp):
            res[s, t] = result[:, t * cols : (t + 1) * cols]

    def send_back(s, first):
        def one(k, c):
            giveback(s, lax.rem(mt + k, tp), me, mt).start()
            return c

        lax.fori_loop(first, tp, one, 0)

    split(me, run(send[me]))
    send_back(me, 1)
    ret[me, mt] = res[me, mt]

    arrive(3)
    arrive(4)

    def index_other(k, c):
        t = lax.rem(mt + k, tp)
        index(t)

        def each(e, c):
            choose(t, e)
            return c

        lax.fori_loop(0, n, each, 0)
        return c

    lax.fori_loop(1, tp, index_other, 0)

    def serve(s):
        dispatch(me, s).wait_recv()
        split(s, run(recv[s]))
        send_back(s, 0)

    def serve_far(j, c):
        serve(far + lax.rem(mine + half - j, half))
        return c

    def serve_near(j, c):
        serve(near + lax.rem(mine + half - j, half))
        return c

    def serve_both(j, c):
        serve_near(j, c)
        return serve_far(j, c)

    serve_far(0, 0)
    lax.fori_loop(1, half, serve_both, 0)

    for load in loads[3:]:
        load.wait()
    arrive(0)
    arrive(1)
    full = (width, sg.shape[2])
    gate_shared = dot(normed[...], sg[...].reshape(full))
    up_shared = dot(normed[...], su[...].reshape(full))
    hidden_all[mt] = (silu(gate_shared) * up_shared).astype(BF16)
    spread(2)

    def placed(e, t):
        ids, gains = routes_all[t], gates_all[t]
        weight = jnp.where(ids[:, 0:1] == e, gains[:, 0:1], 0.0)
        weight = weight + jnp.where(ids[:, 1:2] == e, gains[:, 1:2], 0.0)
        rowsof = lax.dot_general(pick[t, e], ret[e, t], over_rows, preferred_element_type=F32)
        return weight * rowsof

    acc[mt] = placed(me, mt)

    def gather_own(k, c):
        t = lax.rem(mt + tp - k, tp)
        giveback(me, mt, me, t).wait_recv()
        acc[t] = placed(me, t)
        return c

    lax.fori_loop(1, tp, gather_own, 0)

    def gather(e):
        def one(k, c):
            t = lax.rem(mt + tp - k, tp)
            giveback(me, mt, e, t).wait_recv()
            acc[t] += placed(e, t)
            return c

        lax.fori_loop(0, tp, one, 0)

    def gather_far(j, c):
        gather(far + lax.rem(mine + j, half))
        return c

    def gather_near(j, c):
        gather(near + lax.rem(mine + j, half))
        return c

    lax.fori_loop(1, half, gather_near, 0)
    arrive(2)

    def project(t, c):
        shared[t] = dot(hidden_all[t], sd[...]).astype(BF16)
        return c

    lax.fori_loop(0, tp, project, 0)
    lax.fori_loop(0, half, gather_far, 0)

    def total(t, c):
        combined = acc[t].astype(BF16).astype(F32) + shared[t].astype(F32)
        acc[t] = combined
        squares = jnp.sum(combined * combined, axis=1, keepdims=True)
        sums[mt, t] = jnp.broadcast_to(squares, (rows, 128)).T[0:8, :]
        return c

    lax.fori_loop(0, tp, total, 0)
    spread(5)
    arrive(5)

    def finish(t, c):
        squares = sums[0, t]
        for u in range(1, tp):
            squares = squares + sums[u, t]
        squares = jnp.broadcast_to(squares[0:1, :], (128, rows)).T[:, 0:1]
        scale = lax.rsqrt(squares * (1.0 / width) + 1e-06)
        at = pl.ds(pl.multiple_of(t * rows, rows), rows)
        out[at, :] = (acc[t] * scale * post_gain[mt]).astype(BF16)
        return c

    lax.fori_loop(0, tp, finish, 0)

    def drain(d, first):
        def one(k, c):
            giveback(d, lax.rem(mt + k, tp), me, mt).wait_send()
            return c

        lax.fori_loop(first, tp, one, 0)

    def drain_far(j, c):
        d = far + lax.rem(mine + j, half)
        dispatch(d, me).wait_send()
        drain(d, 0)
        return c

    def drain_near(j, c):
        d = near + lax.rem(mine + j, half)
        dispatch(d, me).wait_send()
        drain(d, 0)
        return c

    drain(me, 1)
    lax.fori_loop(0, half, drain_far, 0)
    lax.fori_loop(1, half, drain_near, 0)

    def drain_tp(k, c):
        d = lax.rem(mt + k, tp)
        for which in range(6):
            share(which, d, mt).wait_send()
        return c

    lax.fori_loop(1, tp, drain_tp, 0)


def per_device(
    tokens, routes, gates, pre_gain, w_gate, w_up, w_down, sh_gate, sh_up, sh_down, post_gain
):
    rows, width = tokens.shape
    n = lax.axis_size("ep")
    tp = lax.axis_size("tp")
    cap = -(-max(2, 4 * rows * TOPK // (3 * n)) // 16) * 16
    lanes = -(-n // 128) * 128
    hidden = w_gate.shape[2]
    sh = sh_gate.shape[1]
    cols = width // tp
    vmem = pl.BlockSpec(memory_space=pltpu.VMEM)
    hbm = pl.BlockSpec(memory_space=pl.ANY)
    dma = pltpu.SemaphoreType.DMA
    return pl.pallas_call(
        functools.partial(kernel, n, tp, cap),
        out_shape=jax.ShapeDtypeStruct((tp * rows, cols), BF16),
        in_specs=[vmem] * 5 + [hbm] * 6,
        out_specs=vmem,
        scratch_shapes=[
            pltpu.VMEM((rows, width), BF16),
            pltpu.VMEM((tp, lanes, rows), F32),
            pltpu.VMEM((tp, n, cap, rows), BF16),
            pltpu.VMEM((n, cap, width), BF16),
            pltpu.VMEM((n, cap, width), BF16),
            pltpu.VMEM((n, tp, cap, cols), BF16),
            pltpu.VMEM((n, tp, cap, cols), BF16),
            pltpu.VMEM((width, hidden), BF16),
            pltpu.VMEM((width, hidden), BF16),
            pltpu.VMEM((hidden, width), BF16),
            pltpu.VMEM((tp, width // tp, sh), BF16),
            pltpu.VMEM((tp, width // tp, sh), BF16),
            pltpu.VMEM((sh, cols), BF16),
            pltpu.VMEM((tp, rows, cols), F32),
            pltpu.VMEM((tp, rows, cols), BF16),
            pltpu.VMEM((tp, rows, TOPK), jnp.int32),
            pltpu.VMEM((tp, rows, TOPK), F32),
            pltpu.VMEM((tp, rows, sh), BF16),
            pltpu.VMEM((tp, tp, 8, rows), F32),
            dma((6,)),
            dma((n,)), dma((n,)), dma((n, tp)), dma((n, tp)),
            dma((6, tp)), dma((6, tp)),
        ],
        compiler_params=pltpu.CompilerParams(
            collective_id=0, has_side_effects=True, vmem_limit_bytes=56 * 1024 * 1024
        ),
    )(
        tokens, routes, gates, pre_gain.reshape(1, width), post_gain.reshape(tp, 1, cols),
        w_gate, w_up, w_down, sh_gate, sh_up, sh_down,
    )


def solution(mesh):
    return jax.shard_map(
        per_device,
        mesh=mesh,
        in_specs=(
            P(("ep", "tp"), None),
            P(("ep", "tp"), None),
            P(("ep", "tp"), None),
            P(),
            P("ep", None, None),
            P("ep", None, None),
            P("ep", None, None),
            P("tp", None),
            P("tp", None),
            P(None, "tp"),
            P(),
        ),
        out_specs=P("ep", "tp"),
        check_vma=False,
    )
```
